32 devices in a mesh: grp: 2 (over y), sp: 4 (over z), tp: 4 (over x, core).
Axes of the slice: x: 2, y: 2, z: 4, core: 2. Of those that a mesh axis runs over, the one named last changes fastest.
Arguments:
- recept: bfloat16 [4096, 2048], P(('grp', 'sp'), 'tp'), parts along dimension 0, may hold values from -6 to 6
- key_input: bfloat16 [4096, 2048], P(('grp', 'sp'), 'tp'), parts along dimension 0, may hold values from -6 to 6
- value_input: bfloat16 [4096, 2048], P(('grp', 'sp'), 'tp'), parts along dimension 0, may hold values from -6 to 6
- output_gate_input: bfloat16 [4096, 2048], P(('grp', 'sp'), 'tp'), parts along dimension 0, may hold values from -6 to 6
- decay_input_part: bfloat16 [4096, 2048], P(('grp', 'sp'), 'tp'), parts along dimension 0, may hold values from -4.8 to 4.8
- correction_rate_input: bfloat16 [4096, 2048], P(('grp', 'sp'), 'tp'), parts along dimension 0, may hold values from -4 to 4
- head_decay_offset: float32 [4096, 32], P(('grp', 'sp'), 'tp'), parts along dimension 0, may hold values from -2.1 to 0
- decay_fixed_bias: float32 [2048], P('tp'), may hold values from -11.5 to -2.8
- correction_rate_bias: float32 [2048], P('tp'), may hold values from -8.5 to 1
- head_norm_gain: float32 [2048], P('tp'), may hold values from 0.1 to 1.9
- self_term_weight: float32 [2048], P('tp'), may hold values from -2 to 2
- output_weight_matrix: bfloat16 [2048, 2048], P('tp'), may hold values from -0.125 to 0.125
- residual: bfloat16 [4096, 2048], P(('grp', 'sp', 'tp')), parts along dimension 0, may hold values from -6 to 6
- feedforward_norm_gain: float32 [2048], replicated, may hold values from 0.1 to 1.9
- routed_expert_index: int32 [4096, 2], P(('grp', 'sp', 'tp')), parts along dimension 0, may hold values from 0 to 3, all different within a row; in each aligned block of 128 rows (0 to 127, 128 to 255, ...) at most 96 rows name the same one
- routed_expert_weight: float32 [4096, 2], P(('grp', 'sp', 'tp')), parts along dimension 0, may hold values from 0.2 to 1
- gate_weight_experts: bfloat16 [4, 2048, 1024], P('sp', None, 'tp'), may hold values from -0.125 to 0.125
- up_weight_experts: bfloat16 [4, 2048, 1024], P('sp', None, 'tp'), may hold values from -0.125 to 0.125
- down_weight_experts: bfloat16 [4, 1024, 2048], P('sp', 'tp'), may hold values from -0.1875 to 0.1875
Outputs:
- output: bfloat16 [4096, 2048], P(('grp', 'sp', 'tp')), parts along dimension 0
The draws below stay inside these ranges and needn't reach their ends.
There are 2 independent parts, one for each index of `grp`. The reference program is written for one: setup_inputs(seed, part) draws one part's arguments, and reference() takes and returns one part's arrays. A program takes and returns all parts, laid end to end along the dimension named above; an argument that names none is the same for every part. Nothing has to cross between parts.
Inputs may be any that keep to these rules, and one draw needn't show every extreme that they name: `routed_expert_index`: in each aligned block of 128 rows (the rows of one device) no expert is named by more than 96 routes; the two experts of a row differ.
All inputs are finite; a program needn't handle non-finite values.
Results may differ from the reference program's by a relative error of at most 0.0058.
Values may be sent and summed in bfloat16 or wider, within the bound.
No kernel may reach another device: no remote copies, remote signals or barrier semaphores. Data moves between devices by JAX's collectives and lax.ppermute only.
A program may use at most 128 MiB of HBM per device.

```python
import math
import jax
import jax.numpy as jnp
import numpy as np
from jax import lax

D = 2048
HEAD_COUNT = 32
HEAD_CHANNELS = 64
MODEL_WIDTH = 2048
FF = 1024
EXPERTS = 4
TOK_SP = 512
SEQUENCE_TOKENS = 2048
CAP = 96
N_SP = 4
N_TP = 4


def head_kinds(key):
    share = 5
    fast_heads = jax.random.randint(jax.random.fold_in(key, 11), (HEAD_COUNT,), 0, 10) < share
    return jnp.repeat(fast_heads, HEAD_CHANNELS)


def draw_decay_fixed_bias(key, part):
    fast_chan = head_kinds(key)
    uniform_draw = jax.random.uniform(jax.random.fold_in(key, 12), (MODEL_WIDTH,), jnp.float32)
    return jnp.where(fast_chan, -3.8 + uniform_draw, -11.5 + uniform_draw).astype(jnp.float32)


def draw_correction_rate_bias(key, part):
    fast_chan = head_kinds(key)
    uniform_draw = jax.random.uniform(jax.random.fold_in(key, 13), (MODEL_WIDTH,), jnp.float32)
    return jnp.where(fast_chan, -1.0 + 2.0 * uniform_draw, -8.5 + uniform_draw).astype(jnp.float32)


def draw_decay_input_part(key, part):
    noise = jnp.clip(jax.random.normal(jax.random.fold_in(key, 21), (SEQUENCE_TOKENS, MODEL_WIDTH), jnp.float32), -4.0, 4.0)
    shifts = jax.random.uniform(jax.random.fold_in(key, 22), (SEQUENCE_TOKENS // TOK_SP, 1, 1), jnp.float32, -0.8, 0.8)
    shaped = noise.reshape(SEQUENCE_TOKENS // TOK_SP, TOK_SP, MODEL_WIDTH) + shifts
    return shaped.reshape(SEQUENCE_TOKENS, MODEL_WIDTH).astype(jnp.bfloat16)


def draw_correction_rate_input(key, part):
    noise = jnp.clip(jax.random.normal(jax.random.fold_in(key, 31), (SEQUENCE_TOKENS, MODEL_WIDTH), jnp.float32), -4.0, 4.0)
    return noise.astype(jnp.bfloat16)


def draw_head_decay_offset(key, part):
    spots = jax.random.randint(jax.random.fold_in(key, 41), (3, HEAD_COUNT), 0, SEQUENCE_TOKENS)
    losses = jnp.log(jax.random.uniform(jax.random.fold_in(key, 42), (3, HEAD_COUNT), jnp.float32, 0.5, 0.8))
    places = jnp.arange(SEQUENCE_TOKENS, dtype=jnp.int32)[None, :, None]
    hits = places == spots[:, None, :]
    return jnp.sum(jnp.where(hits, losses[:, None, :], 0.0), axis=0).astype(jnp.float32)


def level_of(rng, dims, split, least, top_value):
    gain, own = 1.0, jax.random.fold_in(rng, 6)
    for dim, blocks in split:
        draws = jnp.exp(jax.random.uniform(jax.random.fold_in(own, dim), (blocks,), jnp.float32, least / len(split), top_value / len(split)))
        gain = gain * jnp.repeat(draws, dims[dim] // blocks).reshape([-1 if axis == dim else 1 for axis in range(len(dims))])
    return gain


def routed_block(rng, own, number, rows, amount, top, most, lean):
    sequence = jax.random.permutation(rng, amount)
    crowded, common = load_shares(amount, rows * top, most, lean, True), load_shares(amount, rows * top, most, lean, False)
    places = jnp.arange(amount)

    def named(sizes, turn):
        used = int((sizes > 0).sum())
        fixed = max(1, used // 4)
        moved = fixed + (places - fixed + turn * (used - fixed)) % max(1, amount - fixed)
        return jnp.zeros((amount,), jnp.int32).at[sequence[jnp.where(places < fixed, places, moved)]].set(jnp.asarray(sizes, jnp.int32))

    sizes = jnp.where(number % 4 == 0, named(crowded, number // 4), named(common, number - number // 4 - 1))
    mixed = jax.random.permutation(jax.random.fold_in(own, 3), amount)
    donor, receiver = mixed[0:amount // 2 * 2:2], mixed[1:amount // 2 * 2:2]
    slack = jnp.minimum(sizes[donor] - 1, most - sizes[receiver]) // 2
    slack = jnp.where((donor == sequence[0]) | (receiver == sequence[0]) | (sizes[receiver] == 0), 0, jnp.maximum(slack, 0))
    moved = jax.random.randint(jax.random.fold_in(own, 4), (amount // 2,), 0, 1 << 20) % (slack + 1)
    sizes = sizes.at[donor].add(-moved).at[receiver].add(moved)
    labels = jnp.searchsorted(jnp.cumsum(sizes), jnp.arange(rows * top), side="right").astype(jnp.int32)
    table = labels.reshape(top, rows).T
    table = table[jax.random.permutation(jax.random.fold_in(own, 1), rows)]
    turn = jax.random.randint(jax.random.fold_in(own, 2), (rows, 1), 0, top)
    return jnp.take_along_axis(table, (jnp.arange(top)[None, :] + turn) % top, axis=1)


def load_shares(count, total, limit, slope, full):
    portions = [(1 << 20) // math.isqrt(rank ** slope) + 1 for rank in range(1, count + 1)]
    largest = limit if full else min(limit, max(-(-total // count), total * portions[0] // sum(portions)))
    least = 1 if total - largest >= count - 1 else 0
    given, surplus = [largest] + [least] * (count - 1), total - largest - least * (count - 1)
    while surplus > 0:
        candidates = [i for i in range(1, count) if given[i] < largest] or [i for i in range(1, count) if given[i] < limit]
        whole, remaining = sum([portions[i] for i in candidates]), surplus
        for i in candidates:
            extra = min(limit - given[i], max(1, remaining * portions[i] // whole), surplus)
            given[i] = given[i] + extra
            surplus = surplus - extra
    return np.array(given)


def bell_draw(stream_key, dims, width, reach, shards=(), held_as=jnp.bfloat16):
    values = jax.random.normal(stream_key, dims, jnp.float32) * width
    if len(shards) > 0:
        values = level_of(stream_key, dims, shards, -0.22, 0.18) * values
    return jnp.clip(values, min=-reach, max=reach).astype(held_as)


def setup_inputs(seed: int = 0, part: int = 0) -> dict:
    streams_of = jax.random.split(jax.random.key(seed), 20)
    own_keys = jax.random.split(jax.random.fold_in(streams_of[19], part), 20)
    recept = bell_draw(own_keys[0], (SEQUENCE_TOKENS, MODEL_WIDTH), 1.0, 6.0, ((0, 4), (1, 4)))
    key_input = bell_draw(own_keys[1], (SEQUENCE_TOKENS, MODEL_WIDTH), 1.0, 6.0, ((0, 4), (1, 4)))
    value_input = bell_draw(own_keys[2], (SEQUENCE_TOKENS, MODEL_WIDTH), 1.0, 6.0, ((0, 4), (1, 4)))
    output_gate_input = bell_draw(own_keys[3], (SEQUENCE_TOKENS, MODEL_WIDTH), 1.0, 6.0, ((0, 4), (1, 4)))
    decay_input_part = draw_decay_input_part(jax.random.fold_in(jax.random.fold_in(streams_of[19], part), 71), part)
    correction_rate_input = draw_correction_rate_input(jax.random.fold_in(jax.random.fold_in(streams_of[19], part), 71), part)
    head_decay_offset = draw_head_decay_offset(jax.random.fold_in(jax.random.fold_in(streams_of[19], part), 71), part)
    decay_fixed_bias = draw_decay_fixed_bias(jax.random.fold_in(streams_of[19], 71), part)
    correction_rate_bias = draw_correction_rate_bias(jax.random.fold_in(streams_of[19], 71), part)
    head_norm_gain = jnp.clip(1.0 + 0.18 * jax.random.normal(streams_of[9], (MODEL_WIDTH,), jnp.float32), 0.1, 1.9)
    self_term_weight = bell_draw(streams_of[10], (MODEL_WIDTH,), 0.15, 2.0, ((0, 4),), jnp.float32)
    output_weight_matrix = bell_draw(streams_of[11], (MODEL_WIDTH, D), MODEL_WIDTH ** -0.5, 0.125, ((0, 4),))
    residual = bell_draw(own_keys[12], (SEQUENCE_TOKENS, D), 1.0, 6.0, ((0, 16),))
    feedforward_norm_gain = jnp.clip(1.0 + 0.18 * jax.random.normal(streams_of[13], (D,), jnp.float32), 0.1, 1.9)
    routed_expert_index_keys = jax.random.split(jax.random.fold_in(own_keys[14], 1), SEQUENCE_TOKENS // (TOK_SP // N_TP))
    routed_expert_index_turns = jax.random.permutation(jax.random.fold_in(own_keys[14], 3), SEQUENCE_TOKENS // (TOK_SP // N_TP))
    routed_expert_index = jax.vmap(lambda own, number: routed_block(jax.random.fold_in(own_keys[14], 2), own, number, TOK_SP // N_TP, EXPERTS, 2, CAP, 1))(routed_expert_index_keys, routed_expert_index_turns).reshape((SEQUENCE_TOKENS, 2))
    routed_expert_weight = jnp.clip(0.2 + 0.8 * jax.random.uniform(own_keys[15], (SEQUENCE_TOKENS, 2), jnp.float32) ** level_of(own_keys[15], (SEQUENCE_TOKENS, 2), ((0, 16),), -0.2, 0.2), 0.2, 1.0)
    gate_weight_experts = bell_draw(streams_of[16], (EXPERTS, D, FF), D ** -0.5, 0.125, ((0, 4), (2, 4)))
    up_weight_experts = bell_draw(streams_of[17], (EXPERTS, D, FF), D ** -0.5, 0.125, ((0, 4), (2, 4)))
    down_weight_experts = bell_draw(streams_of[18], (EXPERTS, FF, D), FF ** -0.5, 0.1875, ((0, 4), (1, 4)))
    return {"recept": recept, "key_input": key_input, "value_input": value_input, "output_gate_input": output_gate_input, "decay_input_part": decay_input_part, "correction_rate_input": correction_rate_input, "head_decay_offset": head_decay_offset, "decay_fixed_bias": decay_fixed_bias, "correction_rate_bias": correction_rate_bias, "head_norm_gain": head_norm_gain, "self_term_weight": self_term_weight, "output_weight_matrix": output_weight_matrix, "residual": residual, "feedforward_norm_gain": feedforward_norm_gain, "routed_expert_index": routed_expert_index, "routed_expert_weight": routed_expert_weight, "gate_weight_experts": gate_weight_experts, "up_weight_experts": up_weight_experts, "down_weight_experts": down_weight_experts}


PRECISE = lax.Precision.HIGHEST
GROUP_EPS = 0.00064
NORM_EPS = 1e-06

def recurrence(receptance_per_head, decay_per_head, key_per_head, value_per_head, remove_h, write_h):

    def advance(states, inputs):
        recept_t, decay_t, key_t, value_t, remove_t, write_t = inputs
        removed = jnp.einsum('hvk,hk->hv', states, remove_t, precision=PRECISE)
        states = states * decay_t[:, None, :] + removed[:, :, None] * write_t[:, None, :] + value_t[:, :, None] * key_t[:, None, :]
        return (states, jnp.einsum('hvk,hk->hv', states, recept_t, precision=PRECISE))
    initial = jnp.zeros((HEAD_COUNT, HEAD_CHANNELS, HEAD_CHANNELS), jnp.float32)
    _, readout = lax.scan(advance, initial, (receptance_per_head, decay_per_head, key_per_head, value_per_head, remove_h, write_h))
    return readout

def expert_rows(features, gate_mat, up_mat, down_mat):
    gated = jnp.dot(features, gate_mat, preferred_element_type=jnp.float32)
    upward = jnp.dot(features, up_mat, preferred_element_type=jnp.float32)
    hidden = (jax.nn.silu(gated) * upward).astype(jnp.bfloat16)
    blocks = jnp.einsum('rjf,jfd->rjd', hidden.reshape(features.shape[0], N_TP, FF // N_TP).astype(jnp.float32), down_mat.reshape(N_TP, FF // N_TP, D).astype(jnp.float32), precision=PRECISE)
    rounded = lax.optimization_barrier(blocks.astype(jnp.bfloat16)).astype(jnp.float32)
    return lax.optimization_barrier(jnp.sum(rounded, axis=1)).astype(jnp.bfloat16)

def reference(recept, key_input, value_input, output_gate_input, decay_input_part, correction_rate_input, head_decay_offset, decay_fixed_bias, correction_rate_bias, head_norm_gain, self_term_weight, output_weight_matrix, residual, feedforward_norm_gain, routed_expert_index, routed_expert_weight, gate_weight_experts, up_weight_experts, down_weight_experts):

    def split_into_heads(tensor):
        return tensor.astype(jnp.float32).reshape(SEQUENCE_TOKENS, HEAD_COUNT, HEAD_CHANNELS)
    receptance_per_head, key_per_head, value_per_head = (split_into_heads(recept), split_into_heads(key_input), split_into_heads(value_input))
    weight_logarithm = -jax.nn.softplus(-(decay_fixed_bias + decay_input_part.astype(jnp.float32))) - 0.5
    decay_per_head = jnp.exp(-jnp.exp(split_into_heads(weight_logarithm)) + head_decay_offset[:, :, None])
    rate_h = split_into_heads(jax.nn.sigmoid(correction_rate_bias + correction_rate_input.astype(jnp.float32)))
    unit_key = key_per_head * lax.rsqrt(lax.optimization_barrier(jnp.sum(key_per_head * key_per_head, axis=-1, keepdims=True)) + NORM_EPS)
    readout = recurrence(receptance_per_head, decay_per_head, key_per_head, value_per_head, -unit_key, unit_key * rate_h)
    center = lax.optimization_barrier(jnp.mean(readout, axis=-1, keepdims=True))
    spread = lax.optimization_barrier(jnp.mean(jnp.square(readout - center), axis=-1, keepdims=True))
    normalized_state = (readout - center) * lax.rsqrt(spread + GROUP_EPS) * head_norm_gain.reshape(HEAD_COUNT, HEAD_CHANNELS)
    self_term = lax.optimization_barrier(jnp.sum(receptance_per_head * key_per_head * self_term_weight.reshape(HEAD_COUNT, HEAD_CHANNELS), axis=-1, keepdims=True)) * value_per_head
    attention_result = ((normalized_state + self_term).reshape(SEQUENCE_TOKENS, MODEL_WIDTH) * output_gate_input.astype(jnp.float32)).astype(jnp.bfloat16)
    proj = jnp.dot(attention_result, output_weight_matrix, preferred_element_type=jnp.float32).astype(jnp.bfloat16)
    stream = residual.astype(jnp.float32) + lax.optimization_barrier(proj).astype(jnp.float32)
    ffn_in = (stream * lax.rsqrt(lax.optimization_barrier(jnp.mean(stream * stream, axis=-1, keepdims=True)) + NORM_EPS) * feedforward_norm_gain).astype(jnp.bfloat16)
    flat_ids = routed_expert_index.reshape(-1).astype(jnp.int32)
    flat_weights = routed_expert_weight.reshape(-1)
    top_count = routed_expert_index.shape[1]
    order = jnp.argsort(flat_ids, stable=True).astype(jnp.int32)
    counts = lax.optimization_barrier(jnp.sum((flat_ids[:, None] == jnp.arange(EXPERTS, dtype=jnp.int32)[None, :]).astype(jnp.int32), axis=0))
    starts = (jnp.cumsum(counts) - counts).astype(jnp.int32)
    room = N_SP * N_TP * CAP
    padded = jnp.concatenate([order, jnp.zeros((room,), jnp.int32)])

    def one_expert(accum, expert):
        entries = lax.dynamic_slice_in_dim(padded, starts[expert], room)
        live = jnp.arange(room, dtype=jnp.int32) < counts[expert]
        positions = (entries // top_count).astype(jnp.int32)
        result = expert_rows(ffn_in[positions], gate_weight_experts[expert], up_weight_experts[expert], down_weight_experts[expert])
        scales = jnp.where(live, flat_weights[entries], 0.0)
        return (accum.at[positions].add(result.astype(jnp.float32) * scales[:, None]), None)
    accum, _ = lax.scan(one_expert, jnp.zeros((SEQUENCE_TOKENS, D), jnp.float32), jnp.arange(EXPERTS, dtype=jnp.int32))
    return (stream + accum).astype(jnp.bfloat16)
```

```python
import functools

import jax
import jax.numpy as jnp
from jax import lax
from jax.experimental import pallas as pl
from jax.experimental.pallas import tpu as pltpu
from jax.sharding import PartitionSpec as P


SPAN = 64


PRECISE = lax.Precision.HIGHEST
GROUP_EPS = 0.00064
NORM_EPS = 1e-06


def dot(left, right, contract=((1,), (0,))):
    return lax.dot_general(
        left.astype(jnp.bfloat16),
        right.astype(jnp.bfloat16),
        (contract, ((), ())),
        preferred_element_type=jnp.float32,
    )


NT = ((1,), (1,))
TN = ((0,), (0,))


def grid_pair(rows, cols):
    return (
        lax.broadcasted_iota(jnp.int32, (rows, cols), 0),
        lax.broadcasted_iota(jnp.int32, (rows, cols), 1),
    )


def head_sums(tensor, width):
    row, col = grid_pair(tensor.shape[1], tensor.shape[1])
    same = (row // width == col // width).astype(jnp.float32)
    return jnp.dot(tensor, same, precision=PRECISE, preferred_element_type=jnp.float32)


def chunk_kernel(
    recept_ref, key_ref, value_ref, decay_ref, rate_ref, offset_ref, bias_ref, rate_bias_ref,
    map_ref, own_ref, total_ref, *, width, pack
):
    group = pl.program_id(0)
    lanes = pack * width
    rows = pack * SPAN
    length = recept_ref.shape[0]
    blocks = length // SPAN
    decay = bias_ref[...] + decay_ref[...].astype(jnp.float32)
    decay_log = -jnp.exp(-jax.nn.softplus(-decay) - 0.5)
    row, col = grid_pair(offset_ref.shape[1], lanes)
    spread = (row == group * pack + col // width).astype(jnp.float32)
    decay_log = decay_log + jnp.dot(
        offset_ref[...], spread, precision=PRECISE, preferred_element_type=jnp.float32
    )
    rate = jax.nn.sigmoid(rate_bias_ref[...] + rate_ref[...].astype(jnp.float32))
    key = key_ref[...].astype(jnp.float32)
    unit_key = key * lax.rsqrt(head_sums(key * key, width) + NORM_EPS)
    recept = recept_ref[...].astype(jnp.float32)
    value = value_ref[...].astype(jnp.float32)

    row, col = grid_pair(SPAN, SPAN)
    ladder = (row >= col).astype(jnp.float32)
    row, col = grid_pair(rows, rows)
    same = row // SPAN == col // SPAN
    strict = same & (row > col)
    within = same & (row >= col)
    eye = (row == col).astype(jnp.float32)
    row, col = grid_pair(rows, lanes)
    mine = row // SPAN == col // width

    def stack(tensor):
        return jnp.where(mine, jnp.concatenate([tensor] * pack, axis=0), 0.0)

    def flat(tensor):
        total = tensor[:SPAN]
        for part in range(1, pack):
            total = total + tensor[part * SPAN : (part + 1) * SPAN]
        return total

    work = []
    for block in range(blocks):
        at = slice(block * SPAN, (block + 1) * SPAN)
        log = decay_log[at]
        cumul = jnp.dot(ladder, log, precision=PRECISE, preferred_element_type=jnp.float32)
        middle = cumul[SPAN // 2 - 1 : SPAN // 2]
        last = cumul[SPAN - 1 : SPAN]
        grow = jnp.exp(middle - cumul)
        remove = stack(-unit_key[at] * jnp.exp(cumul - log - middle))
        read = stack(recept[at] * jnp.exp(cumul - middle))
        write = stack(unit_key[at] * rate[at] * grow)
        keys = stack(key[at] * grow)
        values = stack(value[at])
        scores = dot(
            jnp.concatenate([remove, read], axis=0), jnp.concatenate([write, keys], axis=0), NT
        )
        closing = jnp.exp(last - middle)
        work.append(
            dict(
                remove=remove,
                read=read,
                values=values,
                write=write * closing,
                keys=keys * closing,
                opening=jnp.exp(middle),
                ending=jnp.exp(last),
                rw=jnp.where(strict, scores[:rows, :rows], 0.0),
                rk=jnp.where(strict, scores[:rows, rows:], 0.0),
                qw=jnp.where(within, scores[rows:, :rows], 0.0),
                qk=jnp.where(within, scores[rows:, rows:], 0.0),
            )
        )
    row, col = grid_pair(rows, rows)

    def joint(size):
        return (row // (2 * size) == col // (2 * size)) & (row // size > col // size)

    for w in work:
        w["inverse"] = eye + jnp.where(joint(1), w["rw"], 0.0)
        w["seen"] = dot(w["rk"], w["values"])
    size = 2
    while size < SPAN:
        pick = joint(size)
        for w in work:
            w["half"] = dot(jnp.where(pick, w["rw"], 0.0), w["inverse"])
        for w in work:
            w["inverse"] = w["inverse"] + dot(w["inverse"], w["half"])
        size *= 2
    for w in work:
        w["solved"] = dot(w["inverse"], jnp.concatenate([w["remove"], w["seen"]], axis=1))
        w["own"] = dot(w["qk"], w["values"])
    for w in work:
        answer = dot(w["qw"], w["solved"])
        w["map"] = flat(w["read"] + answer[:, :lanes]) * w["opening"]
        w["own"] = flat(w["own"] + answer[:, lanes:])
        inv_remove = w["solved"][:, :lanes] * w["opening"]
        inv_value = w["solved"][:, lanes:]
        w["move"] = dot(inv_remove, w["write"], TN)
        w["added"] = dot(
            jnp.concatenate([inv_value, w["values"]], axis=0),
            jnp.concatenate([w["write"], w["keys"]], axis=0),
            TN,
        )
    row, col = grid_pair(lanes, lanes)
    transit = (row == col).astype(jnp.float32)
    state = jnp.zeros((lanes, lanes), jnp.float32)
    for block, w in enumerate(work):
        at = slice(block * SPAN, (block + 1) * SPAN)
        both = jnp.concatenate([transit, state], axis=0)
        seen = dot(w["map"], both, NT)
        map_ref[at, :] = seen[:, :lanes].astype(map_ref.dtype)
        own_ref[at, :] = w["own"] + seen[:, lanes:]
        both = both * w["ending"] + dot(both, w["move"])
        transit = both[:lanes]
        state = both[lanes:] + w["added"]

    def compact(tensor):
        total = tensor[:width]
        for part in range(1, pack):
            total = total + tensor[part * width : (part + 1) * width]
        return total

    total_ref[0, :width, :] = compact(transit).astype(total_ref.dtype)
    total_ref[0, width:, :] = compact(state).astype(total_ref.dtype)


def read_kernel(
    place_ref, map_ref, own_ref, totals_ref, recept_ref, key_ref, value_ref, gate_ref, gain_ref,
    self_ref, out_ref, enter_ref, *, width, pack
):
    lanes = pack * width
    row, col = grid_pair(lanes, lanes)
    same = row // width == col // width

    def expand(tensor):
        return jnp.where(same, jnp.concatenate([tensor] * pack, axis=0), 0.0)

    enter_ref[...] = jnp.zeros((lanes, lanes), jnp.float32)

    @pl.loop(0, place_ref[0])
    def _(lap):
        both = totals_ref[lap, 0].astype(jnp.float32)
        enter_ref[...] = dot(enter_ref[...], expand(both[:width])) + expand(both[width:])

    readout = own_ref[...] + dot(map_ref[...], enter_ref[...], NT)
    center = head_sums(readout, width) * (1.0 / width)
    shifted = readout - center
    spread = head_sums(shifted * shifted, width) * (1.0 / width)
    normalized = shifted * lax.rsqrt(spread + GROUP_EPS) * gain_ref[...]
    recept = recept_ref[...].astype(jnp.float32)
    key = key_ref[...].astype(jnp.float32)
    self_term = head_sums(recept * key * self_ref[...], width)
    merged = normalized + self_term * value_ref[...].astype(jnp.float32)
    out_ref[...] = (merged * gate_ref[...].astype(jnp.float32)).astype(jnp.bfloat16)


def mixer(
    recept,
    key_input,
    value_input,
    decay_input_part,
    correction_rate_input,
    head_decay_offset,
    decay_fixed_bias,
    correction_rate_bias,
):
    length, channels = recept.shape
    heads = head_decay_offset.shape[1]
    width = channels // heads
    pack = 2 if heads % 2 == 0 else 1
    lanes = pack * width
    groups = heads // pack
    long = pl.BlockSpec((length, lanes), lambda g: (0, g))
    flat = pl.BlockSpec((1, lanes), lambda g: (0, g))
    readmap, own, total = pl.pallas_call(
        functools.partial(chunk_kernel, width=width, pack=pack),
        grid=(groups,),
        in_specs=[long] * 5 + [pl.BlockSpec((length, heads), lambda g: (0, 0)), flat, flat],
        out_specs=[long, long, pl.BlockSpec((1, 2 * width, lanes), lambda g: (g, 0, 0))],
        out_shape=[
            jax.ShapeDtypeStruct((length, channels), jnp.bfloat16),
            jax.ShapeDtypeStruct((length, channels), jnp.float32),
            jax.ShapeDtypeStruct((groups, 2 * width, lanes), jnp.bfloat16),
        ],
        compiler_params=pltpu.CompilerParams(vmem_limit_bytes=56 * 2**20),
        cost_estimate=pl.CostEstimate(
            flops=40_000_000_000, bytes_accessed=4 * length * channels, transcendentals=0
        ),
        name="chunk_phase",
    )(
        recept, key_input, value_input, decay_input_part, correction_rate_input,
        head_decay_offset, decay_fixed_bias[None], correction_rate_bias[None],
    )
    return readmap, own, total, long, flat, width, pack, groups


def readout_phase(phase, place, totals, recept, key_input, value_input, gate, gain, self_weight):
    readmap, own, total, long, flat, width, pack, groups = phase
    del total
    count = totals.shape[0]
    lanes = pack * width
    return pl.pallas_call(
        functools.partial(read_kernel, width=width, pack=pack),
        grid=(groups,),
        in_specs=[
            pl.BlockSpec(memory_space=pltpu.SMEM),
            long,
            long,
            pl.BlockSpec((count, 1, 2 * width, lanes), lambda g: (0, g, 0, 0)),
            long,
            long,
            long,
            long,
            flat,
            flat,
        ],
        out_specs=long,
        out_shape=jax.ShapeDtypeStruct(own.shape, jnp.bfloat16),
        scratch_shapes=[pltpu.VMEM((lanes, lanes), jnp.float32)],
        compiler_params=pltpu.CompilerParams(vmem_limit_bytes=40 * 2**20),
        name="read_phase",
    )(place, readmap, own, totals, recept, key_input, value_input, gate, gain[None], self_weight[None])


def local(
    recept,
    key_input,
    value_input,
    output_gate_input,
    decay_input_part,
    correction_rate_input,
    head_decay_offset,
    decay_fixed_bias,
    correction_rate_bias,
    head_norm_gain,
    self_term_weight,
    output_weight_matrix,
    residual,
    feedforward_norm_gain,
    routed_expert_index,
    routed_expert_weight,
    gate_weight_experts,
    up_weight_experts,
    down_weight_experts,
):
    experts = gate_weight_experts.shape[0] * lax.axis_size("sp")
    few = experts <= 2 * routed_expert_index.shape[1]
    if few:
        gate_all = lax.all_gather(gate_weight_experts[0], "sp")
        up_all = lax.all_gather(up_weight_experts[0], "sp")
        down_all = lax.all_gather(down_weight_experts[0], "sp")
        named = routed_expert_index[:, :, None] == jnp.arange(experts, dtype=jnp.int32)
        route = jnp.sum(jnp.where(named, routed_expert_weight[:, :, None], 0.0), axis=1)
        route_all = lax.all_gather(route, "tp", axis=0, tiled=True)
    phase = mixer(
        recept,
        key_input,
        value_input,
        decay_input_part,
        correction_rate_input,
        head_decay_offset,
        decay_fixed_bias,
        correction_rate_bias,
    )
    totals = lax.all_gather(phase[2], "sp")
    place = lax.axis_index("sp").astype(jnp.int32).reshape(1)
    attention_result = readout_phase(
        phase,
        place,
        totals,
        recept,
        key_input,
        value_input,
        output_gate_input,
        head_norm_gain,
        self_term_weight,
    )
    partial = jnp.dot(attention_result, output_weight_matrix, preferred_element_type=jnp.float32)
    proj = lax.psum_scatter(
        partial.astype(jnp.bfloat16), "tp", scatter_dimension=0, tiled=True
    )
    stream = residual.astype(jnp.float32) + proj.astype(jnp.float32)
    ffn_in = (
        stream
        * lax.rsqrt(jnp.mean(stream * stream, axis=-1, keepdims=True) + NORM_EPS)
        * feedforward_norm_gain
    ).astype(jnp.bfloat16)
    local_rows = ffn_in.shape[0]
    top_count = routed_expert_index.shape[1]
    experts = gate_weight_experts.shape[0] * lax.axis_size("sp")
    if few:
        rows = lax.all_gather(ffn_in, "tp", axis=0, tiled=True)
        pieces = []
        for e in range(experts):
            gated = jnp.dot(rows, gate_all[e], preferred_element_type=jnp.float32)
            upward = jnp.dot(rows, up_all[e], preferred_element_type=jnp.float32)
            scaled = jax.nn.silu(gated) * upward * route_all[:, e : e + 1]
            pieces.append(scaled.astype(jnp.bfloat16))
        hidden = jnp.concatenate(pieces, axis=1)
        down = down_all.reshape(-1, down_all.shape[-1])
        result = jnp.dot(hidden, down, preferred_element_type=jnp.float32)
        summed = lax.psum_scatter(
            result.astype(jnp.bfloat16), "tp", scatter_dimension=0, tiled=True
        )
        return (stream + summed.astype(jnp.float32)).astype(jnp.bfloat16)
    capacity = max(2, 3 * local_rows // experts)
    flat_ids = routed_expert_index.reshape(-1)
    hits = (flat_ids[:, None] == jnp.arange(experts, dtype=jnp.int32)[None, :]).astype(jnp.int32)
    earlier_hits = jnp.cumsum(hits, axis=0) - hits
    slot_index = jnp.sum(earlier_hits * hits, axis=1)
    target = flat_ids * capacity + slot_index
    places = (target[:, None] == jnp.arange(experts * capacity, dtype=jnp.int32)[None, :]).astype(
        jnp.bfloat16
    )
    places = jnp.sum(places.reshape(local_rows, top_count, experts * capacity), axis=1)
    outgoing = jnp.einsum("rs,rd->sd", places, ffn_in, preferred_element_type=jnp.float32)
    outgoing = outgoing.astype(jnp.bfloat16).reshape(experts, capacity, ffn_in.shape[1])
    incoming = lax.all_gather(
        lax.all_to_all(outgoing, "sp", split_axis=0, concat_axis=0, tiled=True),
        "tp",
        axis=0,
        tiled=True,
    )
    flat = incoming.reshape(-1, incoming.shape[-1])
    gated = jnp.dot(flat, gate_weight_experts[0], preferred_element_type=jnp.float32)
    upward = jnp.dot(flat, up_weight_experts[0], preferred_element_type=jnp.float32)
    hidden = (jax.nn.silu(gated) * upward).astype(jnp.bfloat16)
    result = jnp.dot(hidden, down_weight_experts[0], preferred_element_type=jnp.float32)
    spread_rows = lax.optimization_barrier(
        result.astype(jnp.bfloat16).reshape(incoming.shape)
    ).astype(jnp.float32)
    summed = lax.psum_scatter(
        spread_rows.astype(jnp.bfloat16), "tp", scatter_dimension=0, tiled=True
    )
    expert_out = lax.all_to_all(summed, "sp", split_axis=0, concat_axis=0, tiled=True)
    table = expert_out.reshape(experts * capacity, expert_out.shape[-1])
    fetched = jnp.take(table, target, axis=0).astype(jnp.float32)
    weighted = jnp.sum(
        fetched.reshape(local_rows, top_count, -1) * routed_expert_weight[:, :, None], axis=1
    )
    return (stream + weighted).astype(jnp.bfloat16)


def solution(mesh):
    return jax.shard_map(
        local,
        mesh=mesh,
        in_specs=(
            P(("grp", "sp"), "tp"),
            P(("grp", "sp"), "tp"),
            P(("grp", "sp"), "tp"),
            P(("grp", "sp"), "tp"),
            P(("grp", "sp"), "tp"),
            P(("grp", "sp"), "tp"),
            P(("grp", "sp"), "tp"),
            P("tp"),
            P("tp"),
            P("tp"),
            P("tp"),
            P("tp", None),
            P(("grp", "sp", "tp"), None),
            P(),
            P(("grp", "sp", "tp"), None),
            P(("grp", "sp", "tp"), None),
            P("sp", None, "tp"),
            P("sp", None, "tp"),
            P("sp", "tp", None),
        ),
        out_specs=P(("grp", "sp", "tp"), None),
        check_vma=False,
    )
```

```python
import functools

import jax
import jax.numpy as jnp
from jax import lax
from jax.experimental import pallas as pl
from jax.experimental.pallas import tpu as pltpu
from jax.sharding import PartitionSpec as P


SPAN = 64


PRECISE = lax.Precision.HIGHEST
GROUP_EPS = 0.00064
NORM_EPS = 1e-06


def dot(left, right, contract=((1,), (0,))):
    def once(a, b):
        return lax.dot_general(
            a, b, (contract, ((), ())), preferred_element_type=jnp.float32
        )

    left_high, right_high = left.astype(jnp.bfloat16), right.astype(jnp.bfloat16)
    left_low = (left - left_high.astype(jnp.float32)).astype(jnp.bfloat16)
    right_low = (right - right_high.astype(jnp.float32)).astype(jnp.bfloat16)
    return once(left_high, right_high) + once(left_high, right_low) + once(left_low, right_high)


NT = ((1,), (1,))
TN = ((0,), (0,))


def grid_pair(rows, cols):
    return (
        lax.broadcasted_iota(jnp.int32, (rows, cols), 0),
        lax.broadcasted_iota(jnp.int32, (rows, cols), 1),
    )


def head_sums(tensor, width):
    row, col = grid_pair(tensor.shape[1], tensor.shape[1])
    same = (row // width == col // width).astype(jnp.float32)
    return jnp.dot(tensor, same, precision=PRECISE, preferred_element_type=jnp.float32)


def chunk_kernel(
    recept_ref, key_ref, value_ref, decay_ref, rate_ref, offset_ref, bias_ref, rate_bias_ref,
    map_ref, own_ref, total_ref, *, width, pack
):
    group = pl.program_id(0)
    lanes = pack * width
    rows = pack * SPAN
    length = recept_ref.shape[0]
    blocks = length // SPAN
    decay = bias_ref[...] + decay_ref[...].astype(jnp.float32)
    decay_log = -jnp.exp(-jax.nn.softplus(-decay) - 0.5)
    row, col = grid_pair(offset_ref.shape[1], lanes)
    spread = (row == group * pack + col // width).astype(jnp.float32)
    decay_log = decay_log + jnp.dot(
        offset_ref[...], spread, precision=PRECISE, preferred_element_type=jnp.float32
    )
    rate = jax.nn.sigmoid(rate_bias_ref[...] + rate_ref[...].astype(jnp.float32))
    key = key_ref[...].astype(jnp.float32)
    unit_key = key * lax.rsqrt(head_sums(key * key, width) + NORM_EPS)
    recept = recept_ref[...].astype(jnp.float32)
    value = value_ref[...].astype(jnp.float32)

    row, col = grid_pair(SPAN, SPAN)
    ladder = (row >= col).astype(jnp.float32)
    row, col = grid_pair(rows, rows)
    same = row // SPAN == col // SPAN
    strict = same & (row > col)
    within = same & (row >= col)
    eye = (row == col).astype(jnp.float32)
    row, col = grid_pair(rows, lanes)
    mine = row // SPAN == col // width

    def stack(tensor):
        return jnp.where(mine, jnp.concatenate([tensor] * pack, axis=0), 0.0)

    def flat(tensor):
        total = tensor[:SPAN]
        for part in range(1, pack):
            total = total + tensor[part * SPAN : (part + 1) * SPAN]
        return total

    work = []
    for block in range(blocks):
        at = slice(block * SPAN, (block + 1) * SPAN)
        log = decay_log[at]
        cumul = jnp.dot(ladder, log, precision=PRECISE, preferred_element_type=jnp.float32)
        middle = cumul[SPAN // 2 - 1 : SPAN // 2]
        last = cumul[SPAN - 1 : SPAN]
        grow = jnp.exp(middle - cumul)
        remove = stack(-unit_key[at] * jnp.exp(cumul - log - middle))
        read = stack(recept[at] * jnp.exp(cumul - middle))
        write = stack(unit_key[at] * rate[at] * grow)
        keys = stack(key[at] * grow)
        values = stack(value[at])
        scores = dot(
            jnp.concatenate([remove, read], axis=0), jnp.concatenate([write, keys], axis=0), NT
        )
        closing = jnp.exp(last - middle)
        work.append(
            dict(
                remove=remove,
                read=read,
                values=values,
                write=write * closing,
                keys=keys * closing,
                opening=jnp.exp(middle),
                ending=jnp.exp(last),
                rw=jnp.where(strict, scores[:rows, :rows], 0.0),
                rk=jnp.where(strict, scores[:rows, rows:], 0.0),
                qw=jnp.where(within, scores[rows:, :rows], 0.0),
                qk=jnp.where(within, scores[rows:, rows:], 0.0),
            )
        )
    row, col = grid_pair(rows, rows)

    def joint(size):
        return (row // (2 * size) == col // (2 * size)) & (row // size > col // size)

    for w in work:
        w["inverse"] = eye + jnp.where(joint(1), w["rw"], 0.0)
        w["seen"] = dot(w["rk"], w["values"])
    size = 2
    while size < SPAN:
        pick = joint(size)
        for w in work:
            w["half"] = dot(jnp.where(pick, w["rw"], 0.0), w["inverse"])
        for w in work:
            w["inverse"] = w["inverse"] + dot(w["inverse"], w["half"])
        size *= 2
    for w in work:
        w["solved"] = dot(w["inverse"], jnp.concatenate([w["remove"], w["seen"]], axis=1))
        w["own"] = dot(w["qk"], w["values"])
    for w in work:
        answer = dot(w["qw"], w["solved"])
        w["map"] = flat(w["read"] + answer[:, :lanes]) * w["opening"]
        w["own"] = flat(w["own"] + answer[:, lanes:])
        inv_remove = w["solved"][:, :lanes] * w["opening"]
        inv_value = w["solved"][:, lanes:]
        w["move"] = dot(inv_remove, w["write"], TN)
        w["added"] = dot(
            jnp.concatenate([inv_value, w["values"]], axis=0),
            jnp.concatenate([w["write"], w["keys"]], axis=0),
            TN,
        )
    row, col = grid_pair(lanes, lanes)
    transit = (row == col).astype(jnp.float32)
    state = jnp.zeros((lanes, lanes), jnp.float32)
    for block, w in enumerate(work):
        at = slice(block * SPAN, (block + 1) * SPAN)
        both = jnp.concatenate([transit, state], axis=0)
        seen = dot(w["map"], both, NT)
        map_ref[at, :] = seen[:, :lanes].astype(map_ref.dtype)
        own_ref[at, :] = w["own"] + seen[:, lanes:]
        both = both * w["ending"] + dot(both, w["move"])
        transit = both[:lanes]
        state = both[lanes:] + w["added"]

    def compact(tensor):
        total = tensor[:width]
        for part in range(1, pack):
            total = total + tensor[part * width : (part + 1) * width]
        return total

    total_ref[0, :width, :] = compact(transit).astype(total_ref.dtype)
    total_ref[0, width:, :] = compact(state).astype(total_ref.dtype)


def read_kernel(
    place_ref, map_ref, own_ref, totals_ref, recept_ref, key_ref, value_ref, gate_ref, gain_ref,
    self_ref, out_ref, enter_ref, *, width, pack
):
    lanes = pack * width
    row, col = grid_pair(lanes, lanes)
    same = row // width == col // width

    def expand(tensor):
        return jnp.where(same, jnp.concatenate([tensor] * pack, axis=0), 0.0)

    enter_ref[...] = jnp.zeros((lanes, lanes), jnp.float32)

    @pl.loop(0, place_ref[0])
    def _(lap):
        both = totals_ref[lap, 0].astype(jnp.float32)
        enter_ref[...] = dot(enter_ref[...], expand(both[:width])) + expand(both[width:])

    readout = own_ref[...] + dot(map_ref[...], enter_ref[...], NT)
    center = head_sums(readout, width) * (1.0 / width)
    shifted = readout - center
    spread = head_sums(shifted * shifted, width) * (1.0 / width)
    normalized = shifted * lax.rsqrt(spread + GROUP_EPS) * gain_ref[...]
    recept = recept_ref[...].astype(jnp.float32)
    key = key_ref[...].astype(jnp.float32)
    self_term = head_sums(recept * key * self_ref[...], width)
    merged = normalized + self_term * value_ref[...].astype(jnp.float32)
    out_ref[...] = (merged * gate_ref[...].astype(jnp.float32)).astype(jnp.bfloat16)


def mixer(
    recept,
    key_input,
    value_input,
    decay_input_part,
    correction_rate_input,
    head_decay_offset,
    decay_fixed_bias,
    correction_rate_bias,
):
    length, channels = recept.shape
    heads = head_decay_offset.shape[1]
    width = channels // heads
    pack = 2 if heads % 2 == 0 else 1
    lanes = pack * width
    groups = heads // pack
    long = pl.BlockSpec((length, lanes), lambda g: (0, g))
    flat = pl.BlockSpec((1, lanes), lambda g: (0, g))
    readmap, own, total = pl.pallas_call(
        functools.partial(chunk_kernel, width=width, pack=pack),
        grid=(groups,),
        in_specs=[long] * 5 + [pl.BlockSpec((length, heads), lambda g: (0, 0)), flat, flat],
        out_specs=[long, long, pl.BlockSpec((1, 2 * width, lanes), lambda g: (g, 0, 0))],
        out_shape=[
            jax.ShapeDtypeStruct((length, channels), jnp.float32),
            jax.ShapeDtypeStruct((length, channels), jnp.float32),
            jax.ShapeDtypeStruct((groups, 2 * width, lanes), jnp.bfloat16),
        ],
        compiler_params=pltpu.CompilerParams(vmem_limit_bytes=56 * 2**20),
        cost_estimate=pl.CostEstimate(
            flops=40_000_000_000, bytes_accessed=4 * length * channels, transcendentals=0
        ),
        name="chunk_phase",
    )(
        recept, key_input, value_input, decay_input_part, correction_rate_input,
        head_decay_offset, decay_fixed_bias[None], correction_rate_bias[None],
    )
    return readmap, own, total, long, flat, width, pack, groups


def readout_phase(phase, place, totals, recept, key_input, value_input, gate, gain, self_weight):
    readmap, own, total, long, flat, width, pack, groups = phase
    del total
    count = totals.shape[0]
    lanes = pack * width
    return pl.pallas_call(
        functools.partial(read_kernel, width=width, pack=pack),
        grid=(groups,),
        in_specs=[
            pl.BlockSpec(memory_space=pltpu.SMEM),
            long,
            long,
            pl.BlockSpec((count, 1, 2 * width, lanes), lambda g: (0, g, 0, 0)),
            long,
            long,
            long,
            long,
            flat,
            flat,
        ],
        out_specs=long,
        out_shape=jax.ShapeDtypeStruct(own.shape, jnp.bfloat16),
        scratch_shapes=[pltpu.VMEM((lanes, lanes), jnp.float32)],
        compiler_params=pltpu.CompilerParams(vmem_limit_bytes=40 * 2**20),
        name="read_phase",
    )(place, readmap, own, totals, recept, key_input, value_input, gate, gain[None], self_weight[None])


def local(
    recept,
    key_input,
    value_input,
    output_gate_input,
    decay_input_part,
    correction_rate_input,
    head_decay_offset,
    decay_fixed_bias,
    correction_rate_bias,
    head_norm_gain,
    self_term_weight,
    output_weight_matrix,
    residual,
    feedforward_norm_gain,
    routed_expert_index,
    routed_expert_weight,
    gate_weight_experts,
    up_weight_experts,
    down_weight_experts,
):
    experts = gate_weight_experts.shape[0] * lax.axis_size("sp")
    few = (
        experts <= 2 * routed_expert_index.shape[1]
        and experts == lax.axis_size("sp")
        and lax.axis_size("grp") == 2
        and gate_weight_experts.shape[2] % 256 == 0
    )
    if few:
        half = gate_weight_experts.shape[2] // 2
        group = lax.axis_index("grp")
        place = lax.axis_index("sp")

        def fetch(weight, axis):
            near = lax.dynamic_slice_in_dim(weight, group * half, half, axis)
            far = lax.dynamic_slice_in_dim(weight, (1 - group) * half, half, axis)
            gathered = lax.all_gather(near, "sp")
            blocks = [gathered[e] for e in range(experts)] + [far]
            for step in range(1, experts):
                chosen = lax.dynamic_index_in_dim(gathered, (place + step) % experts, 0, False)
                blocks.append(lax.ppermute(chosen, "grp", [(0, 1), (1, 0)]))
            return gathered, blocks

        _, gate_blocks = fetch(gate_weight_experts[0], 1)
        _, up_blocks = fetch(up_weight_experts[0], 1)
        down_all, down_blocks = fetch(down_weight_experts[0], 0)
        named = routed_expert_index[:, :, None] == jnp.arange(experts, dtype=jnp.int32)
        route = jnp.sum(jnp.where(named, routed_expert_weight[:, :, None], 0.0), axis=1)
        route_all = lax.all_gather(route, "tp", axis=0, tiled=True)
    phase = mixer(
        recept,
        key_input,
        value_input,
        decay_input_part,
        correction_rate_input,
        head_decay_offset,
        decay_fixed_bias,
        correction_rate_bias,
    )
    totals = lax.all_gather(phase[2], "sp")
    place = lax.axis_index("sp").astype(jnp.int32).reshape(1)
    attention_result = readout_phase(
        phase,
        place,
        totals,
        recept,
        key_input,
        value_input,
        output_gate_input,
        head_norm_gain,
        self_term_weight,
    )
    partial = jnp.dot(attention_result, output_weight_matrix, preferred_element_type=jnp.float32)
    proj = lax.psum_scatter(
        partial.astype(jnp.bfloat16), "tp", scatter_dimension=0, tiled=True
    )
    stream = residual.astype(jnp.float32) + proj.astype(jnp.float32)
    ffn_in = (
        stream
        * lax.rsqrt(jnp.mean(stream * stream, axis=-1, keepdims=True) + NORM_EPS)
        * feedforward_norm_gain
    ).astype(jnp.bfloat16)
    local_rows = ffn_in.shape[0]
    top_count = routed_expert_index.shape[1]
    experts = gate_weight_experts.shape[0] * lax.axis_size("sp")
    if few:
        rows = lax.all_gather(ffn_in, "tp", axis=0, tiled=True)
        pieces = []
        for at in range(2 * experts):
            gated = jnp.dot(rows, gate_blocks[at], preferred_element_type=jnp.float32)
            upward = jnp.dot(rows, up_blocks[at], preferred_element_type=jnp.float32)
            expert = at if at < experts else (place + at - experts) % experts
            mine = jnp.arange(experts, dtype=jnp.int32)[None, :] == expert
            share = jnp.sum(jnp.where(mine, route_all, 0.0), axis=1, keepdims=True)
            pieces.append((jax.nn.silu(gated) * upward * share).astype(jnp.bfloat16))
        hidden = jnp.concatenate(pieces, axis=1)
        down = jnp.concatenate([down_all.reshape(-1, rows.shape[1])] + down_blocks[experts:], axis=0)
        result = jnp.dot(hidden, down, preferred_element_type=jnp.float32)
        summed = lax.psum_scatter(
            result.astype(jnp.bfloat16), "tp", scatter_dimension=0, tiled=True
        )
        return (stream + summed.astype(jnp.float32)).astype(jnp.bfloat16)
    capacity = max(2, 3 * local_rows // experts)
    flat_ids = routed_expert_index.reshape(-1)
    hits = (flat_ids[:, None] == jnp.arange(experts, dtype=jnp.int32)[None, :]).astype(jnp.int32)
    earlier_hits = jnp.cumsum(hits, axis=0) - hits
    slot_index = jnp.sum(earlier_hits * hits, axis=1)
    target = flat_ids * capacity + slot_index
    places = (target[:, None] == jnp.arange(experts * capacity, dtype=jnp.int32)[None, :]).astype(
        jnp.bfloat16
    )
    places = jnp.sum(places.reshape(local_rows, top_count, experts * capacity), axis=1)
    outgoing = jnp.einsum("rs,rd->sd", places, ffn_in, preferred_element_type=jnp.float32)
    outgoing = outgoing.astype(jnp.bfloat16).reshape(experts, capacity, ffn_in.shape[1])
    incoming = lax.all_gather(
        lax.all_to_all(outgoing, "sp", split_axis=0, concat_axis=0, tiled=True),
        "tp",
        axis=0,
        tiled=True,
    )
    flat = incoming.reshape(-1, incoming.shape[-1])
    gated = jnp.dot(flat, gate_weight_experts[0], preferred_element_type=jnp.float32)
    upward = jnp.dot(flat, up_weight_experts[0], preferred_element_type=jnp.float32)
    hidden = (jax.nn.silu(gated) * upward).astype(jnp.bfloat16)
    result = jnp.dot(hidden, down_weight_experts[0], preferred_element_type=jnp.float32)
    spread_rows = lax.optimization_barrier(
        result.astype(jnp.bfloat16).reshape(incoming.shape)
    ).astype(jnp.float32)
    summed = lax.psum_scatter(
        spread_rows.astype(jnp.bfloat16), "tp", scatter_dimension=0, tiled=True
    )
    expert_out = lax.all_to_all(summed, "sp", split_axis=0, concat_axis=0, tiled=True)
    table = expert_out.reshape(experts * capacity, expert_out.shape[-1])
    fetched = jnp.take(table, target, axis=0).astype(jnp.float32)
    weighted = jnp.sum(
        fetched.reshape(local_rows, top_count, -1) * routed_expert_weight[:, :, None], axis=1
    )
    return (stream + weighted).astype(jnp.bfloat16)


def solution(mesh):
    return jax.shard_map(
        local,
        mesh=mesh,
        in_specs=(
            P(("grp", "sp"), "tp"),
            P(("grp", "sp"), "tp"),
            P(("grp", "sp"), "tp"),
            P(("grp", "sp"), "tp"),
            P(("grp", "sp"), "tp"),
            P(("grp", "sp"), "tp"),
            P(("grp", "sp"), "tp"),
            P("tp"),
            P("tp"),
            P("tp"),
            P("tp"),
            P("tp", None),
            P(("grp", "sp", "tp"), None),
            P(),
            P(("grp", "sp", "tp"), None),
            P(("grp", "sp", "tp"), None),
            P("sp", None, "tp"),
            P("sp", None, "tp"),
            P("sp", "tp", None),
        ),
        out_specs=P(("grp", "sp", "tp"), None),
        check_vma=False,
    )
```
